32 devices in a mesh: sp: 8 (over z, x), tp: 4 (over y, core).
Axes of the slice: x: 2, y: 2, z: 4, core: 2. Of those that a mesh axis runs over, the one named last changes fastest.
Arguments:
- x_resid: bfloat16 [1024, 2048], P(('sp', 'tp')), may hold values from -3 to 3
- query_proj: bfloat16 [1024, 2048], P('sp', 'tp'), may hold values from -6 to 6
- projected_key_heads: bfloat16 [1024, 1024], P('sp', 'tp'), may hold values from -6 to 6
- projected_value_heads: bfloat16 [1024, 1024], P('sp', 'tp'), may hold values from -6 to 6
- query_gain: float32 [128], replicated, may hold values from 1.3 to 6.5
- key_norm_gain: float32 [128], replicated, may hold values from 1.3 to 6.5
- out_weight: bfloat16 [2048, 2048], P('tp'), may hold values from -0.125 to 0.125
- ffn_gain: float32 [2048], replicated, may hold values from 0.1 to 1.9
- routing: int32 [1024, 2], P(('sp', 'tp')), may hold values from 0 to 7, all different within a row; in each aligned block of 32 rows (0 to 31, 32 to 63, ...) at most 16 rows name the same one
- route_scores: float32 [1024, 2], P(('sp', 'tp')), may hold values from -6 to 6
- expert_gate: bfloat16 [8, 2048, 4096], P('sp', None, 'tp'), may hold values from -0.125 to 0.125
- expert_up: bfloat16 [8, 2048, 4096], P('sp', None, 'tp'), may hold values from -0.125 to 0.125
- expert_down: bfloat16 [8, 4096, 2048], P('sp', 'tp'), may hold values from -0.09375 to 0.09375
Outputs:
- layer_out: bfloat16 [1024, 2048], P(('sp', 'tp'))
The draws below stay inside these ranges and needn't reach their ends.
Inputs may be any that keep to these rules, and one draw needn't show every extreme that they name: `routing`: each row names 2 different experts. In each aligned block of 32 rows (the rows of one device) no expert is named by more than 16 rows, a bound that some block reaches.
All inputs are finite; a program needn't handle non-finite values.
Results may differ from the reference program's by a relative error of at most 0.018.
The reference program's roundings to bfloat16 on the way count: a program that leaves them out, or rounds other values in their place, can miss the bound.
Values may be sent and summed in bfloat16 or wider, within the bound.
A program may use at most 128 MiB of HBM per device.

```python
import math
import jax
import jax.numpy as jnp
import numpy as np
from jax import lax

D = 2048
HEAD_WIDTH = 128
QUERY_HEADS = 16
KEY_VALUE_HEADS = 8
FF = 4096
TOP = 2
GRID_W = 64
TOK_DEV = 32
TOKEN_COUNT = 1024
EXPERTS = 8
CAP = 16
N_SP = 8
N_TP = 4


def draw_pair(key):
    base_key = jax.random.fold_in(key, 7)
    query_key, random_key_seed = jax.random.split(base_key, 2)
    query_rows = jax.random.normal(query_key, (TOKEN_COUNT, QUERY_HEADS, HEAD_WIDTH), jnp.float32)
    every_key_row = jax.random.normal(random_key_seed, (TOKEN_COUNT, KEY_VALUE_HEADS, HEAD_WIDTH), jnp.float32)
    query_rows = jnp.clip(query_rows, -6.0, 6.0)
    every_key_row = jnp.clip(every_key_row, -6.0, 6.0)
    return (query_rows.reshape(TOKEN_COUNT, QUERY_HEADS * HEAD_WIDTH), every_key_row.reshape(TOKEN_COUNT, KEY_VALUE_HEADS * HEAD_WIDTH))


def draw_query_proj(key, part):
    return draw_pair(key)[0].astype(jnp.bfloat16)


def draw_projected_key_heads(key, part):
    return draw_pair(key)[1].astype(jnp.bfloat16)


def draw_gains(key, salt):
    values = jax.random.uniform(jax.random.fold_in(key, salt), (HEAD_WIDTH,), jnp.float32)
    return 1.3 + 0.6 * values


def draw_query_gain(key, part):
    return draw_gains(key, 11)


def draw_key_norm_gain(key, part):
    return draw_gains(key, 13)


def block_scale(own_key, extent, cuts, smallest, high):
    level, own = 1.0, jax.random.fold_in(own_key, 6)
    for position, shards_of in cuts:
        steps = jnp.exp(jax.random.uniform(jax.random.fold_in(own, position), (shards_of,), jnp.float32, smallest / len(cuts), high / len(cuts)))
        level = level * jnp.repeat(steps, extent[position] // shards_of).reshape([-1 if axis == position else 1 for axis in range(len(extent))])
    return level


def assign_block(stream_key, own, number, rows, count, top, limit, skew):
    order = jax.random.permutation(stream_key, count)
    packed, common = load_shares(count, rows * top, limit, skew, True), load_shares(count, rows * top, limit, skew, False)
    places = jnp.arange(count)

    def named(sizes, offset_by):
        used = int((sizes > 0).sum())
        fixed = max(1, used // 4)
        shifted = fixed + (places - fixed + offset_by * (used - fixed)) % max(1, count - fixed)
        return jnp.zeros((count,), jnp.int32).at[order[jnp.where(places < fixed, places, shifted)]].set(jnp.asarray(sizes, jnp.int32))

    sizes = jnp.where(number % 4 == 0, named(packed, number // 4), named(common, number - number // 4 - 1))
    mixed = jax.random.permutation(jax.random.fold_in(own, 3), count)
    source_of, receiver = mixed[0:count // 2 * 2:2], mixed[1:count // 2 * 2:2]
    slack = jnp.minimum(sizes[source_of] - 1, limit - sizes[receiver]) // 2
    slack = jnp.where((source_of == order[0]) | (receiver == order[0]) | (sizes[receiver] == 0), 0, jnp.maximum(slack, 0))
    shifted = jax.random.randint(jax.random.fold_in(own, 4), (count // 2,), 0, 1 << 20) % (slack + 1)
    sizes = sizes.at[source_of].add(-shifted).at[receiver].add(shifted)
    items = jnp.searchsorted(jnp.cumsum(sizes), jnp.arange(rows * top), side="right").astype(jnp.int32)
    grid = items.reshape(top, rows).T
    grid = grid[jax.random.permutation(jax.random.fold_in(own, 1), rows)]
    offset_by = jax.random.randint(jax.random.fold_in(own, 2), (rows, 1), 0, top)
    return jnp.take_along_axis(grid, (jnp.arange(top)[None, :] + offset_by) % top, axis=1)


def load_shares(number_of, total, bound, slope, full):
    weights = [(1 << 20) // math.isqrt(rank ** slope) + 1 for rank in range(1, number_of + 1)]
    largest = bound if full else min(bound, max(-(-total // number_of), total * weights[0] // sum(weights)))
    least = 1 if total - largest >= number_of - 1 else 0
    given, rest = [largest] + [least] * (number_of - 1), total - largest - least * (number_of - 1)
    while rest > 0:
        movable = [i for i in range(1, number_of) if given[i] < largest] or [i for i in range(1, number_of) if given[i] < bound]
        whole, left = sum([weights[i] for i in movable]), rest
        for i in movable:
            addition = min(bound - given[i], max(1, left * weights[i] // whole), rest)
            given[i] = given[i] + addition
            rest = rest - addition
    return np.array(given)


def centred(stream_key, extent, scale, bound, shards=(), kind=jnp.bfloat16):
    loudness = block_scale(stream_key, extent, shards, -0.22, 0.18) if shards else 1.0
    drawn = jax.random.normal(stream_key, extent, jnp.float32) * scale * loudness
    return jnp.minimum(jnp.maximum(drawn, -bound), bound).astype(kind)


def setup_inputs(seed: int = 0) -> dict:
    key_of = jax.random.split(jax.random.key(seed), 14)
    x_resid = centred(key_of[0], (TOKEN_COUNT, D), 0.5, 3.0, ((0, 32),))
    query_proj = draw_query_proj(jax.random.fold_in(key_of[13], 71), 0)
    projected_key_heads = draw_projected_key_heads(jax.random.fold_in(key_of[13], 71), 0)
    projected_value_heads = centred(key_of[3], (TOKEN_COUNT, KEY_VALUE_HEADS * HEAD_WIDTH), 1.0, 6.0, ((0, 8), (1, 4)))
    query_gain = draw_query_gain(jax.random.fold_in(key_of[13], 71), 0)
    key_norm_gain = draw_key_norm_gain(jax.random.fold_in(key_of[13], 71), 0)
    out_weight = centred(key_of[6], (QUERY_HEADS * HEAD_WIDTH, D), (QUERY_HEADS * HEAD_WIDTH) ** -0.5, 0.125, ((0, 4),))
    ffn_gain = jnp.clip(1.0 + 0.18 * jax.random.normal(key_of[7], (D,), jnp.float32), 0.1, 1.9)
    routing_keys = jax.random.split(jax.random.fold_in(key_of[8], 1), TOKEN_COUNT // TOK_DEV)
    routing_turns = jax.random.permutation(jax.random.fold_in(key_of[8], 3), TOKEN_COUNT // TOK_DEV)
    routing = jax.vmap(lambda own, number: assign_block(jax.random.fold_in(key_of[8], 2), own, number, TOK_DEV, EXPERTS, TOP, CAP, 2))(routing_keys, routing_turns).reshape((TOKEN_COUNT, TOP))
    route_scores = centred(key_of[9], (TOKEN_COUNT, TOP), 1.5, 6.0, ((0, 32),), jnp.float32)
    expert_gate = centred(key_of[10], (EXPERTS, D, FF), D ** -0.5, 0.125, ((0, 8), (2, 4)))
    expert_up = centred(key_of[11], (EXPERTS, D, FF), D ** -0.5, 0.125, ((0, 8), (2, 4)))
    expert_down = centred(key_of[12], (EXPERTS, FF, D), FF ** -0.5, 0.09375, ((0, 8), (1, 4)))
    return {"x_resid": x_resid, "query_proj": query_proj, "projected_key_heads": projected_key_heads, "projected_value_heads": projected_value_heads, "query_gain": query_gain, "key_norm_gain": key_norm_gain, "out_weight": out_weight, "ffn_gain": ffn_gain, "routing": routing, "route_scores": route_scores, "expert_gate": expert_gate, "expert_up": expert_up, "expert_down": expert_down}


NORM_EPS = 1e-06
ROPE_BASE = 10000.0

def rms_scale(values, norm_gain):
    return values * lax.rsqrt(lax.optimization_barrier(jnp.mean(values * values, axis=-1, keepdims=True)) + NORM_EPS) * norm_gain

def grid_angles(token_positions, head_size):
    freq_count = head_size // 4
    frequency = ROPE_BASE ** (-jnp.arange(freq_count, dtype=jnp.float32) / freq_count)
    grid_row = (token_positions // GRID_W).astype(jnp.float32)
    grid_col = (token_positions % GRID_W).astype(jnp.float32)
    return (grid_row[:, None] * frequency, grid_col[:, None] * frequency)

def turn_half(values, angles):
    cosine = jnp.cos(angles)[:, None, :]
    sine_part = jnp.sin(angles)[:, None, :]
    leading, trailing = jnp.split(values, 2, axis=-1)
    return jnp.concatenate([leading * cosine - trailing * sine_part, trailing * cosine + leading * sine_part], axis=-1)

def normalize_rotate(projected, norm_gain, token_positions, heads):
    length = projected.shape[0]
    values = projected.astype(jnp.float32).reshape(length, heads, -1)
    head_size = values.shape[-1]
    values = rms_scale(values, norm_gain)
    row_angle, col_angle = grid_angles(token_positions, head_size)
    half_size = head_size // 2
    turned = jnp.concatenate([turn_half(values[..., :half_size], row_angle), turn_half(values[..., half_size:], col_angle)], axis=-1)
    return turned.reshape(length, heads * head_size).astype(jnp.bfloat16)

def reference(x_resid, query_proj, projected_key_heads, projected_value_heads, query_gain, key_norm_gain, out_weight, ffn_gain, routing, route_scores, expert_gate, expert_up, expert_down):
    token_positions = jnp.arange(TOKEN_COUNT, dtype=jnp.int32)
    query_rows = normalize_rotate(query_proj, query_gain, token_positions, QUERY_HEADS)
    rotated_key_rows = normalize_rotate(projected_key_heads, key_norm_gain, token_positions, KEY_VALUE_HEADS)
    head_groups = QUERY_HEADS // KEY_VALUE_HEADS
    rows_per_block = math.gcd(TOKEN_COUNT, 256)
    blocks_of_queries = query_rows.reshape(TOKEN_COUNT // rows_per_block, rows_per_block, KEY_VALUE_HEADS, head_groups, HEAD_WIDTH)
    grid_of_keys = rotated_key_rows.reshape(TOKEN_COUNT, KEY_VALUE_HEADS, HEAD_WIDTH).astype(jnp.float32)
    grid_of_values = projected_value_heads.reshape(TOKEN_COUNT, KEY_VALUE_HEADS, HEAD_WIDTH).astype(jnp.float32)

    def attend(query_block):
        scores = jnp.einsum('qhgd,khd->hgqk', query_block.astype(jnp.float32), grid_of_keys) * HEAD_WIDTH ** (-0.5)
        row_top = lax.optimization_barrier(jnp.max(scores, axis=-1, keepdims=True))
        weights = jnp.exp(scores - row_top)
        total = lax.optimization_barrier(jnp.sum(weights, axis=-1))
        rounded = lax.optimization_barrier(weights.astype(jnp.bfloat16)).astype(jnp.float32)
        summed = jnp.einsum('hgqk,khd->qhgd', rounded, grid_of_values)
        return (summed / jnp.transpose(total, (2, 0, 1))[..., None]).astype(jnp.bfloat16)
    attended = lax.map(attend, blocks_of_queries).reshape(TOKEN_COUNT, QUERY_HEADS * HEAD_WIDTH)
    col_width = QUERY_HEADS * HEAD_WIDTH // N_TP
    proj_sum = jnp.zeros((TOKEN_COUNT, D), jnp.float32)
    for block_index in range(N_TP):
        low_col = block_index * col_width
        partial_value = jnp.dot(attended[:, low_col:low_col + col_width], out_weight[low_col:low_col + col_width], preferred_element_type=jnp.float32)
        proj_sum = proj_sum + lax.optimization_barrier(partial_value.astype(jnp.bfloat16)).astype(jnp.float32)
    attn_proj = lax.optimization_barrier(proj_sum.astype(jnp.bfloat16)).astype(jnp.float32)
    middle = x_resid.astype(jnp.float32) + attn_proj
    normed = rms_scale(middle, ffn_gain).astype(jnp.bfloat16)
    flat_expert = routing.reshape(-1).astype(jnp.int32)
    assigned = flat_expert.shape[0]
    flat_token = jnp.arange(assigned, dtype=jnp.int32) // TOP
    flat_gate = jax.nn.softmax(route_scores.astype(jnp.float32), axis=-1).reshape(-1)
    sort_order = jnp.argsort(flat_expert, stable=True)
    sorted_token = flat_token[sort_order]
    sorted_gate = flat_gate[sort_order]
    counts = lax.optimization_barrier(jnp.sum((flat_expert[None, :] == jnp.arange(EXPERTS, dtype=jnp.int32)[:, None]).astype(jnp.int32), axis=1))
    starts = jnp.cumsum(counts) - counts
    most_rows = N_SP * N_TP * CAP
    slot_index = jnp.arange(most_rows, dtype=jnp.int32)
    hidden_width = FF // N_TP

    def run_expert(operands):
        gate_matrix, up_matrix, down_matrix, expert_index = operands
        filled = slot_index < counts[expert_index]
        where_rows = jnp.minimum(starts[expert_index] + slot_index, assigned - 1).astype(jnp.int32)
        token_ids = sorted_token[where_rows]
        inputs = normed[token_ids]
        gate_part = jnp.dot(inputs, gate_matrix, preferred_element_type=jnp.float32)
        up_part = jnp.dot(inputs, up_matrix, preferred_element_type=jnp.float32)
        hidden = (jax.nn.silu(gate_part) * up_part).astype(jnp.bfloat16)
        summed = jnp.zeros((most_rows, D), jnp.float32)
        for block_index in range(N_TP):
            low_row = block_index * hidden_width
            partial_value = jnp.dot(hidden[:, low_row:low_row + hidden_width], down_matrix[low_row:low_row + hidden_width], preferred_element_type=jnp.float32)
            summed = summed + lax.optimization_barrier(partial_value.astype(jnp.bfloat16)).astype(jnp.float32)
        expert_result = lax.optimization_barrier(summed.astype(jnp.bfloat16)).astype(jnp.float32)
        weight = jnp.where(filled, sorted_gate[where_rows], jnp.zeros((most_rows,), jnp.float32))
        targets = jnp.where(filled, token_ids, jnp.full((most_rows,), TOKEN_COUNT, jnp.int32))
        return (expert_result * weight[:, None], targets)
    contrib, targets = lax.map(run_expert, (expert_gate, expert_up, expert_down, jnp.arange(EXPERTS, dtype=jnp.int32)))
    routed = jax.ops.segment_sum(contrib.reshape(-1, D), targets.reshape(-1), num_segments=TOKEN_COUNT + 1)[:TOKEN_COUNT]
    return (middle + routed).astype(jnp.bfloat16)
```

```python
import functools
import math

import jax
import jax.numpy as jnp
from jax import lax
from jax.experimental import pallas as pl
from jax.experimental.pallas import tpu as pltpu
from jax.sharding import PartitionSpec as P

MESH = pl.DeviceIdType.MESH

HEAD_WIDTH = 128
TOP = 2
GRID_W = 64


NORM_EPS = 1e-06
ROPE_BASE = 10000.0
NEG_LARGE = -1e30


def rms_scale(values, norm_gain):
    return (
        values * lax.rsqrt(jnp.mean(values * values, axis=-1, keepdims=True) + NORM_EPS) * norm_gain
    )


def grid_angles(token_positions, head_size):
    freq_count = head_size // 4
    frequency = ROPE_BASE ** (-jnp.arange(freq_count, dtype=jnp.float32) / freq_count)
    grid_row = (token_positions // GRID_W).astype(jnp.float32)
    grid_col = (token_positions % GRID_W).astype(jnp.float32)
    return (grid_row[:, None] * frequency, grid_col[:, None] * frequency)


def turn_half(values, angles):
    cosine = jnp.cos(angles)[:, None, :]
    sine_part = jnp.sin(angles)[:, None, :]
    leading, trailing = jnp.split(values, 2, axis=-1)
    return jnp.concatenate(
        [leading * cosine - trailing * sine_part, trailing * cosine + leading * sine_part], axis=-1
    )


def normalize_rotate(projected, norm_gain, token_positions, heads):
    length = projected.shape[0]
    values = projected.astype(jnp.float32).reshape(length, heads, -1)
    head_size = values.shape[-1]
    values = rms_scale(values, norm_gain)
    row_angle, col_angle = grid_angles(token_positions, head_size)
    half_size = head_size // 2
    turned = jnp.concatenate(
        [
            turn_half(values[..., :half_size], row_angle),
            turn_half(values[..., half_size:], col_angle),
        ],
        axis=-1,
    )
    return turned.reshape(length, heads * head_size).astype(jnp.bfloat16)


def local_plain(
    x_resid,
    query_proj,
    projected_key_heads,
    projected_value_heads,
    query_gain,
    key_norm_gain,
    out_weight,
    ffn_gain,
    routing,
    route_scores,
    expert_gate,
    expert_up,
    expert_down,
):
    seq_rows = query_proj.shape[0]
    q_heads = query_proj.shape[1] // HEAD_WIDTH
    kv_heads = projected_key_heads.shape[1] // HEAD_WIDTH
    head_groups = q_heads // kv_heads
    token_positions = lax.axis_index("sp") * seq_rows + jnp.arange(seq_rows, dtype=jnp.int32)
    query_rows = normalize_rotate(query_proj, query_gain, token_positions, q_heads)
    rotated_key_rows = normalize_rotate(
        projected_key_heads, key_norm_gain, token_positions, kv_heads
    )
    query_grid = query_rows.reshape(seq_rows, kv_heads, head_groups, HEAD_WIDTH)
    score_scale = HEAD_WIDTH ** (-0.5)
    run_max = jnp.full((kv_heads, head_groups, seq_rows), NEG_LARGE, jnp.float32)
    key_piece = lax.all_gather(rotated_key_rows, "sp", axis=0, tiled=True).reshape(
        -1, kv_heads, HEAD_WIDTH
    )
    value_piece = lax.all_gather(projected_value_heads, "sp", axis=0, tiled=True).reshape(
        -1, kv_heads, HEAD_WIDTH
    )
    scores = (
        jnp.einsum("qhgd,khd->hgqk", query_grid, key_piece, preferred_element_type=jnp.float32)
        * score_scale
    )
    new_max = jnp.maximum(run_max, jnp.max(scores, axis=-1))
    weights = jnp.exp(scores - new_max[..., None])
    new_total = jnp.sum(weights, axis=-1)
    addition = jnp.einsum(
        "hgqk,khd->hgqd",
        weights.astype(jnp.bfloat16),
        value_piece,
        preferred_element_type=jnp.float32,
    )
    attended = (
        (addition / new_total[..., None])
        .transpose(2, 0, 1, 3)
        .reshape(seq_rows, q_heads * HEAD_WIDTH)
        .astype(jnp.bfloat16)
    )
    own_tokens = x_resid.shape[0]
    model_width = x_resid.shape[1]
    row_block = attended
    attn_proj = lax.psum_scatter(
        jnp.dot(row_block, out_weight, preferred_element_type=jnp.float32).astype(jnp.bfloat16),
        "tp",
        scatter_dimension=0,
        tiled=True,
    )
    middle = x_resid.astype(jnp.float32) + attn_proj.astype(jnp.float32)
    normed = rms_scale(middle, ffn_gain).astype(jnp.bfloat16)
    experts_all = lax.axis_size("sp") * expert_gate.shape[0]
    capacity = max(2, 2 * own_tokens * TOP // experts_all)
    flat_expert = routing.reshape(-1)
    one_hot = (flat_expert[:, None] == jnp.arange(experts_all, dtype=jnp.int32)[None, :]).astype(
        jnp.int32
    )
    earlier = jnp.cumsum(one_hot, axis=0) - one_hot
    slot_rank = jnp.sum(earlier * one_hot, axis=1)
    target = flat_expert * capacity + slot_rank
    chooser = (
        jnp.arange(experts_all * capacity, dtype=jnp.int32)[:, None] == target[None, :]
    ).astype(jnp.float32)
    gate_share = jax.nn.softmax(route_scores, axis=-1).reshape(-1)
    picker = jnp.sum(chooser.reshape(experts_all * capacity, own_tokens, TOP), axis=2).astype(
        jnp.bfloat16
    )
    combiner = jnp.sum(
        (chooser * gate_share[None, :]).reshape(experts_all * capacity, own_tokens, TOP), axis=2
    )
    dispatch = (
        jnp.dot(picker, normed, preferred_element_type=jnp.float32)
        .astype(jnp.bfloat16)
        .reshape(experts_all, capacity, model_width)
    )
    gate_matrix = expert_gate[0]
    up_matrix = expert_up[0]
    down_matrix = expert_down[0]
    arrived = lax.all_to_all(dispatch, "sp", split_axis=0, concat_axis=0, tiled=True)
    row_block = lax.all_gather(arrived.reshape(-1, model_width), "tp", axis=0, tiled=True)
    gate_part = jnp.dot(row_block, gate_matrix, preferred_element_type=jnp.float32)
    up_part = jnp.dot(row_block, up_matrix, preferred_element_type=jnp.float32)
    hidden = (jax.nn.silu(gate_part) * up_part).astype(jnp.bfloat16)
    row_block = hidden
    expert_result = lax.psum_scatter(
        jnp.dot(row_block, down_matrix, preferred_element_type=jnp.float32).astype(jnp.bfloat16),
        "tp",
        scatter_dimension=0,
        tiled=True,
    )
    returned = lax.all_to_all(
        expert_result.reshape(-1, capacity, model_width),
        "sp",
        split_axis=0,
        concat_axis=0,
        tiled=True,
    )
    routed = jnp.einsum(
        "st,sd->td",
        combiner,
        returned.reshape(-1, model_width).astype(jnp.float32),
        precision=lax.Precision.HIGHEST,
    )
    return (middle + routed).astype(jnp.bfloat16)


def rdma(src, dst, send_sem, recv_sem, device):
    return pltpu.make_async_remote_copy(
        src_ref=src,
        dst_ref=dst,
        send_sem=send_sem,
        recv_sem=recv_sem,
        device_id=device,
        device_id_type=MESH,
    )


def turn_head(values, gain, cosine, sine):
    values = values * lax.rsqrt(jnp.mean(values * values, axis=-1, keepdims=True) + NORM_EPS) * gain
    width = values.shape[1]
    quarter = width // 4
    lane = lax.broadcasted_iota(jnp.int32, values.shape, 1)
    swapped = jnp.where(
        lane % (2 * quarter) < quarter,
        pltpu.roll(values, width - quarter, 1),
        pltpu.roll(values, quarter, 1),
    )
    return (values * cosine + swapped * sine).astype(jnp.bfloat16)


def hop_order(count):
    order = [0]
    for distance in range(1, count // 2 + 1):
        order.append(distance)
        if count - distance != distance:
            order.append(count - distance)
    return order


def layer_kernel(
    n_sp,
    n_tp,
    capacity,
    q_ref,
    k_ref,
    v_ref,
    cos_ref,
    sin_ref,
    qg_ref,
    kg_ref,
    x_ref,
    fg_ref,
    route_ref,
    score_ref,
    ow_hbm,
    wg_hbm,
    wu_hbm,
    wd_hbm,
    out_ref,
    kbuf,
    vbuf,
    qs,
    att,
    part,
    rsbuf,
    mid,
    disp,
    rows,
    hid,
    eo,
    cor,
    pair,
    yrec,
    res,
    ret,
    ow,
    wg,
    wu,
    wd,
    w_sem,
    k_s,
    k_r,
    v_s,
    v_r,
    rs_s,
    rs_r,
    d_s,
    rows_r,
    y_s,
    c_s,
    e_s,
    e_r,
    p_s,
    p_r,
    b_s,
    b_r,
):
    s = lax.axis_index("sp")
    t = lax.axis_index("tp")
    n_x = math.isqrt(n_sp // 2)
    if n_x == 0 or n_sp % n_x:
        n_x = 1
    n_z = n_sp // n_x
    z, x = s // n_x, s % n_x
    n_y = n_tp // 2
    y, c = t // 2, t % 2
    core_peer = (s, y * 2 + 1 - c)
    order = hop_order(n_sp)
    seq_rows, q_width = q_ref.shape
    kv_width = k_ref.shape[1]
    q_heads, kv_heads = q_width // HEAD_WIDTH, kv_width // HEAD_WIDTH
    groups = q_heads // kv_heads
    own, model = x_ref.shape
    f_width = wg.shape[1]
    pending = []

    def send(src, dst, send_sem, recv_sem, device):
        copy = rdma(src, dst, send_sem, recv_sem, device)
        copy.start()
        pending.append(copy)

    def arrive(dst, recv_sem):
        rdma(dst, dst, recv_sem, recv_sem, core_peer).wait_recv()

    weight_copies = [
        pltpu.make_async_copy(ow_hbm, ow, w_sem.at[0]),
        pltpu.make_async_copy(wg_hbm.at[0], wg, w_sem.at[1]),
        pltpu.make_async_copy(wu_hbm.at[0], wu, w_sem.at[2]),
        pltpu.make_async_copy(wd_hbm.at[0], wd, w_sem.at[3]),
    ]
    for copy in weight_copies:
        copy.start()

    barrier = pltpu.get_barrier_semaphore()
    for d in range(1, n_sp):
        pl.semaphore_signal(barrier, inc=1, device_id=((s + d) % n_sp, t), device_id_type=MESH)
    for d in range(1, n_tp):
        pl.semaphore_signal(barrier, inc=1, device_id=(s, (t + d) % n_tp), device_id_type=MESH)

    cosine, sine = cos_ref[...], sin_ref[...]
    for h in range(kv_heads):
        cols = slice(h * HEAD_WIDTH, (h + 1) * HEAD_WIDTH)
        kbuf[0, :, cols] = turn_head(k_ref[:, cols].astype(jnp.float32), kg_ref[...], cosine, sine)
    pl.semaphore_wait(barrier, n_sp - 1 + n_tp - 1)

    for buf, first, s_sem, r_sem in ((kbuf, kbuf.at[0], k_s, k_r), (vbuf, v_ref, v_s, v_r)):
        for dx in range(1, n_x):
            send(first, buf.at[dx], s_sem.at[dx], r_sem.at[dx], (z * n_x + (x + dx) % n_x, t))
        for dz in range(1, n_z):
            slot = dz * n_x
            peer = ((z + dz) % n_z) * n_x + x
            send(first, buf.at[slot], s_sem.at[slot], r_sem.at[slot], (peer, t))
    vbuf[0] = v_ref[...]
    for h in range(q_heads):
        cols = slice(h * HEAD_WIDTH, (h + 1) * HEAD_WIDTH)
        kv, member = h // groups, h % groups
        qs[kv, member * seq_rows : (member + 1) * seq_rows, :] = turn_head(
            q_ref[:, cols].astype(jnp.float32), qg_ref[...], cosine, sine
        )
    total_slots = n_sp * capacity
    lane = lax.broadcasted_iota(jnp.int32, (own, total_slots), 1)
    lane_place = lane // capacity
    lane_expert = jnp.zeros_like(lane)
    for k, d in enumerate(order):
        lane_expert = jnp.where(lane_place == k, (s + d) % n_sp, lane_expert)
    first_hit = route_ref[:, 0:1] == lane_expert
    named = first_hit | (route_ref[:, 1:2] == lane_expert)
    earlier = (
        lax.broadcasted_iota(jnp.int32, (own, own), 1)
        < lax.broadcasted_iota(jnp.int32, (own, own), 0)
    )
    rank = jnp.dot(
        earlier.astype(jnp.float32).astype(jnp.bfloat16),
        named.astype(jnp.float32).astype(jnp.bfloat16),
        preferred_element_type=jnp.float32,
    )
    picked = jnp.where(
        named & (rank == (lane % capacity).astype(jnp.float32)), 1.0, 0.0
    )
    route_scores = score_ref[...]
    share = jnp.exp(route_scores - jnp.max(route_scores, axis=-1, keepdims=True))
    share = share / jnp.sum(share, axis=-1, keepdims=True)
    combiner = picked * jnp.where(first_hit, share[:, 0:1], share[:, 1:2])
    picker = picked.astype(jnp.bfloat16)

    for buf, s_sem, r_sem in ((kbuf, k_s, k_r), (vbuf, v_s, v_r)):
        for dz in range(1, n_z):
            slot = dz * n_x
            arrive(buf.at[slot], r_sem.at[slot])
            for dx in range(1, n_x):
                send(
                    buf.at[slot],
                    buf.at[slot + dx],
                    s_sem.at[slot + dx],
                    r_sem.at[slot + dx],
                    (z * n_x + (x + dx) % n_x, t),
                )
    for slot in range(n_sp):
        if slot % n_x:
            arrive(kbuf.at[slot], k_r.at[slot])
    keys_all = n_sp * seq_rows
    score_scale = HEAD_WIDTH ** (-0.5)
    heads_done = []
    for kv in range(kv_heads):
        cols = slice(kv * HEAD_WIDTH, (kv + 1) * HEAD_WIDTH)
        keys = kbuf[:, :, cols].reshape(keys_all, HEAD_WIDTH)
        scores = (
            lax.dot_general(
                qs[kv], keys, (((1,), (1,)), ((), ())), preferred_element_type=jnp.float32
            )
            * score_scale
        )
        weights = jnp.exp(scores - jnp.max(scores, axis=-1, keepdims=True))
        total = jnp.sum(weights, axis=-1, keepdims=True)
        heads_done.append((weights.astype(jnp.bfloat16), total))
    for slot in range(n_sp):
        if slot % n_x:
            arrive(vbuf.at[slot], v_r.at[slot])
    for kv in range(kv_heads):
        cols = slice(kv * HEAD_WIDTH, (kv + 1) * HEAD_WIDTH)
        values = vbuf[:, :, cols].reshape(keys_all, HEAD_WIDTH)
        weights, total = heads_done[kv]
        mixed = jnp.dot(weights, values, preferred_element_type=jnp.float32) / total
        for member in range(groups):
            h = kv * groups + member
            att[:, h * HEAD_WIDTH : (h + 1) * HEAD_WIDTH] = mixed[
                member * seq_rows : (member + 1) * seq_rows
            ].astype(jnp.bfloat16)

    weight_copies[0].wait()
    tile = min(512, model)
    for j in range(model // tile):
        cols = slice(j * tile, (j + 1) * tile)
        part[:, :, cols] = (
            jnp.dot(att[...], ow[:, cols], preferred_element_type=jnp.float32)
            .astype(jnp.bfloat16)
            .reshape(n_tp, own, tile)
        )
    for d in range(n_tp - 1, 0, -1):
        peer = (t + d) % n_tp
        send(part.at[peer], rsbuf.at[d], rs_s.at[d], rs_r.at[d], (s, peer))
    summed = part[t].astype(jnp.float32)
    for d in range(1, n_tp):
        arrive(rsbuf.at[d], rs_r.at[d])
        summed = summed + rsbuf[d].astype(jnp.float32)
    middle = x_ref[...].astype(jnp.float32) + summed.astype(jnp.bfloat16).astype(jnp.float32)
    mid[...] = middle
    normed = (
        middle
        * lax.rsqrt(jnp.mean(middle * middle, axis=-1, keepdims=True) + NORM_EPS)
        * fg_ref[...]
    ).astype(jnp.bfloat16)
    chosen = (
        lax.dot_general(
            picker, normed, (((0,), (0,)), ((), ())), preferred_element_type=jnp.float32
        )
        .astype(jnp.bfloat16)
        .reshape(n_sp, capacity, model)
    )
    disp[...] = chosen
    for k, d in enumerate(order):
        if k:
            send(disp.at[k], rows.at[k, t], d_s.at[k], rows_r.at[k, t], ((s + d) % n_sp, t))
    rows[0, t] = chosen[0]

    def forward(k):
        if k:
            arrive(rows.at[k, t], rows_r.at[k, t])
        for dy in range(1, n_y):
            peer = ((y + dy) % n_y) * 2 + c
            send(rows.at[k, t], rows.at[k, t], y_s.at[k, dy], rows_r.at[k, t], (s, peer))
        send(rows.at[k, t], rows.at[k, t], c_s.at[k, 0], rows_r.at[k, t], core_peer)

    def relay(k):
        for dy in range(1, n_y):
            source = ((y + n_y - dy) % n_y) * 2 + c
            arrive(rows.at[k, source], rows_r.at[k, source])
            send(
                rows.at[k, source],
                rows.at[k, source],
                c_s.at[k, dy],
                rows_r.at[k, source],
                core_peer,
            )

    def settle(k):
        for dy in range(n_y):
            source = ((y + n_y - dy) % n_y) * 2 + 1 - c
            arrive(rows.at[k, source], rows_r.at[k, source])

    n_groups = 2
    group = n_sp // n_groups
    group_rows = group * n_tp * capacity

    def give_pair(g):
        ks = pl.ds(g * group, group)
        send(eo.at[1 - c, :, ks], cor.at[:, ks], e_s.at[g], e_r.at[g], core_peer)

    def sum_pair(g):
        ks = pl.ds(g * group, group)
        arrive(cor.at[:, ks], e_r.at[g])
        for dy in range(1, n_y):
            far = (y + dy) % n_y
            pair[dy, ks] = (
                eo[c, far, ks].astype(jnp.float32) + cor[far, ks].astype(jnp.float32)
            ).astype(jnp.bfloat16)
            send(
                pair.at[dy, ks], yrec.at[dy, ks], p_s.at[g, dy], p_r.at[g, dy], (s, far * 2 + c)
            )

    def give_back(g):
        ks = pl.ds(g * group, group)
        for dy in range(1, n_y):
            arrive(yrec.at[dy, ks], p_r.at[g, dy])
        for k in range(g * group, (g + 1) * group):
            whole = eo[c, y, k].astype(jnp.float32) + cor[y, k].astype(jnp.float32)
            for dy in range(1, n_y):
                whole = whole + yrec[dy, k].astype(jnp.float32)
            if k == 0:
                ret[0] = whole.astype(jnp.bfloat16)
            else:
                res[k] = whole.astype(jnp.bfloat16)
                peer = (s + n_sp - order[k]) % n_sp
                send(res.at[k], ret.at[k], b_s.at[k], b_r.at[k], (peer, t))

    def experts(g, hooks):
        hooks = list(hooks)
        block = rows[g * group : (g + 1) * group].reshape(group_rows, model)
        f_tile = min(256, f_width)
        for j in range(f_width // f_tile):
            cols = slice(j * f_tile, (j + 1) * f_tile)
            gate = jnp.dot(block, wg[:, cols], preferred_element_type=jnp.float32)
            up = jnp.dot(block, wu[:, cols], preferred_element_type=jnp.float32)
            hid[:, cols] = (gate / (1.0 + jnp.exp(-gate)) * up).astype(jnp.bfloat16)
            if hooks:
                hooks.pop(0)()
        if g == 0:
            weight_copies[3].wait()
        for j in range(model // tile):
            cols = slice(j * tile, (j + 1) * tile)
            down = jnp.dot(hid[...], wd[:, cols], preferred_element_type=jnp.float32)
            down = down.astype(jnp.bfloat16).reshape(group, n_y, 2, capacity, tile)
            for core in range(2):
                for far in range(n_y):
                    eo[core, far, g * group : (g + 1) * group, :, cols] = down[:, far, core]
            if hooks:
                hooks.pop(0)()
        for hook in hooks:
            hook()

    for k in range(group):
        forward(k)
    for k in range(group):
        relay(k)
    for k in range(group):
        settle(k)
    weight_copies[1].wait()
    weight_copies[2].wait()
    late = range(group, n_sp)
    experts(
        0,
        [functools.partial(forward, k) for k in late] + [functools.partial(relay, k) for k in late],
    )
    give_pair(0)
    for k in late:
        settle(k)
    nothing = lambda: None
    experts(
        1,
        [
            functools.partial(sum_pair, 0),
            nothing,
            nothing,
            nothing,
            functools.partial(give_back, 0),
        ],
    )
    give_pair(1)
    sum_pair(1)
    give_back(1)
    for k in range(1, n_sp):
        arrive(ret.at[k], b_r.at[k])
    high = combiner.astype(jnp.bfloat16)
    rest = combiner - high.astype(jnp.float32)
    middle_part = rest.astype(jnp.bfloat16)
    low = (rest - middle_part.astype(jnp.float32)).astype(jnp.bfloat16)
    returned = ret[...].reshape(total_slots, model)
    routed = jnp.dot(
        jnp.concatenate([high, middle_part, low], axis=0),
        returned,
        preferred_element_type=jnp.float32,
    )
    routed = routed[:own] + routed[own : 2 * own] + routed[2 * own :]
    out_ref[...] = (mid[...] + routed).astype(jnp.bfloat16)
    for copy in pending:
        copy.wait_send()


def rope_tables(token_positions):
    row_angle, col_angle = grid_angles(token_positions, HEAD_WIDTH)
    angles = jnp.concatenate([row_angle, row_angle, col_angle, col_angle], axis=1)
    quarter = HEAD_WIDTH // 4
    sign = jnp.where(jnp.arange(HEAD_WIDTH) % (2 * quarter) < quarter, -1.0, 1.0)
    return jnp.cos(angles), jnp.sin(angles) * sign.astype(jnp.float32)


def local(
    x_resid,
    query_proj,
    projected_key_heads,
    projected_value_heads,
    query_gain,
    key_norm_gain,
    out_weight,
    ffn_gain,
    routing,
    route_scores,
    expert_gate,
    expert_up,
    expert_down,
):
    n_sp, n_tp = lax.axis_size("sp"), lax.axis_size("tp")
    own, model = x_resid.shape
    experts_all = n_sp * expert_gate.shape[0]
    capacity = max(2, 2 * own * TOP // experts_all)
    if capacity % 16 or n_tp % 2 or n_sp % 2 or expert_gate.shape[0] != 1:
        return local_plain(
            x_resid,
            query_proj,
            projected_key_heads,
            projected_value_heads,
            query_gain,
            key_norm_gain,
            out_weight,
            ffn_gain,
            routing,
            route_scores,
            expert_gate,
            expert_up,
            expert_down,
        )
    seq_rows, q_width = query_proj.shape
    kv_width = projected_key_heads.shape[1]
    kv_heads = kv_width // HEAD_WIDTH
    groups = q_width // kv_width
    f_width = expert_gate.shape[2]
    n_y = n_tp // 2
    token_positions = lax.axis_index("sp") * seq_rows + jnp.arange(seq_rows, dtype=jnp.int32)
    cosine, sine = rope_tables(token_positions)
    bf16 = jnp.bfloat16
    dma = pltpu.SemaphoreType.DMA
    vmem = pl.BlockSpec(memory_space=pltpu.VMEM)
    hbm = pl.BlockSpec(memory_space=pl.ANY)
    return pl.pallas_call(
        functools.partial(layer_kernel, n_sp, n_tp, capacity),
        out_shape=jax.ShapeDtypeStruct((own, model), bf16),
        in_specs=[vmem] * 11 + [hbm] * 4,
        out_specs=vmem,
        scratch_shapes=[
            pltpu.VMEM((n_sp, seq_rows, kv_width), bf16),
            pltpu.VMEM((n_sp, seq_rows, kv_width), bf16),
            pltpu.VMEM((kv_heads, groups * seq_rows, HEAD_WIDTH), bf16),
            pltpu.VMEM((seq_rows, q_width), bf16),
            pltpu.VMEM((n_tp, own, model), bf16),
            pltpu.VMEM((n_tp, own, model), bf16),
            pltpu.VMEM((own, model), jnp.float32),
            pltpu.VMEM((n_sp, capacity, model), bf16),
            pltpu.VMEM((n_sp, n_tp, capacity, model), bf16),
            pltpu.VMEM((n_sp // 2 * n_tp * capacity, f_width), bf16),
            pltpu.VMEM((2, n_y, n_sp, capacity, model), bf16),
            pltpu.VMEM((n_y, n_sp, capacity, model), bf16),
            pltpu.VMEM((n_y, n_sp, capacity, model), bf16),
            pltpu.VMEM((n_y, n_sp, capacity, model), bf16),
            pltpu.VMEM((n_sp, capacity, model), bf16),
            pltpu.VMEM((n_sp, capacity, model), bf16),
            pltpu.VMEM(out_weight.shape, bf16),
            pltpu.VMEM(expert_gate.shape[1:], bf16),
            pltpu.VMEM(expert_up.shape[1:], bf16),
            pltpu.VMEM(expert_down.shape[1:], bf16),
            dma((4,)),
            dma((n_sp,)),
            dma((n_sp,)),
            dma((n_sp,)),
            dma((n_sp,)),
            dma((n_tp,)),
            dma((n_tp,)),
            dma((n_sp,)),
            dma((n_sp, n_tp)),
            dma((n_sp, n_y)),
            dma((n_sp, n_y)),
            dma((2,)),
            dma((2,)),
            dma((2, n_y)),
            dma((2, n_y)),
            dma((n_sp,)),
            dma((n_sp,)),
        ],
        compiler_params=pltpu.CompilerParams(
            collective_id=0, has_side_effects=True, vmem_limit_bytes=56 * 1024 * 1024
        ),
    )(
        query_proj,
        projected_key_heads,
        projected_value_heads,
        cosine,
        sine,
        query_gain.reshape(1, -1),
        key_norm_gain.reshape(1, -1),
        x_resid,
        ffn_gain.reshape(1, -1),
        routing,
        route_scores,
        out_weight,
        expert_gate,
        expert_up,
        expert_down,
    )


def solution(mesh):
    in_specs = (
        P(("sp", "tp"), None),
        P("sp", "tp"),
        P("sp", "tp"),
        P("sp", "tp"),
        P(),
        P(),
        P("tp", None),
        P(),
        P(("sp", "tp"), None),
        P(("sp", "tp"), None),
        P("sp", None, "tp"),
        P("sp", None, "tp"),
        P("sp", "tp", None),
    )
    out_specs = P(("sp", "tp"), None)
    return jax.shard_map(local, mesh=mesh, in_specs=in_specs, out_specs=out_specs, check_vma=False)
```

```python
import functools
import math

import jax
import jax.numpy as jnp
import numpy as np
from jax import lax
from jax.experimental import pallas as pl
from jax.experimental.pallas import tpu as pltpu
from jax.sharding import PartitionSpec as P

MESH = pl.DeviceIdType.MESH

HEAD_WIDTH = 128
TOP = 2
GRID_W = 64


NORM_EPS = 1e-06
ROPE_BASE = 10000.0
NEG_LARGE = -1e30


def rms_scale(values, norm_gain):
    return (
        values * lax.rsqrt(jnp.mean(values * values, axis=-1, keepdims=True) + NORM_EPS) * norm_gain
    )


def grid_angles(token_positions, head_size):
    freq_count = head_size // 4
    frequency = ROPE_BASE ** (-jnp.arange(freq_count, dtype=jnp.float32) / freq_count)
    grid_row = (token_positions // GRID_W).astype(jnp.float32)
    grid_col = (token_positions % GRID_W).astype(jnp.float32)
    return (grid_row[:, None] * frequency, grid_col[:, None] * frequency)


def turn_half(values, angles):
    cosine = jnp.cos(angles)[:, None, :]
    sine_part = jnp.sin(angles)[:, None, :]
    leading, trailing = jnp.split(values, 2, axis=-1)
    return jnp.concatenate(
        [leading * cosine - trailing * sine_part, trailing * cosine + leading * sine_part], axis=-1
    )


def normalize_rotate(projected, norm_gain, token_positions, heads):
    length = projected.shape[0]
    values = projected.astype(jnp.float32).reshape(length, heads, -1)
    head_size = values.shape[-1]
    values = rms_scale(values, norm_gain)
    row_angle, col_angle = grid_angles(token_positions, head_size)
    half_size = head_size // 2
    turned = jnp.concatenate(
        [
            turn_half(values[..., :half_size], row_angle),
            turn_half(values[..., half_size:], col_angle),
        ],
        axis=-1,
    )
    return turned.reshape(length, heads * head_size).astype(jnp.bfloat16)


def local_plain(
    x_resid,
    query_proj,
    projected_key_heads,
    projected_value_heads,
    query_gain,
    key_norm_gain,
    out_weight,
    ffn_gain,
    routing,
    route_scores,
    expert_gate,
    expert_up,
    expert_down,
):
    seq_rows = query_proj.shape[0]
    q_heads = query_proj.shape[1] // HEAD_WIDTH
    kv_heads = projected_key_heads.shape[1] // HEAD_WIDTH
    head_groups = q_heads // kv_heads
    token_positions = lax.axis_index("sp") * seq_rows + jnp.arange(seq_rows, dtype=jnp.int32)
    query_rows = normalize_rotate(query_proj, query_gain, token_positions, q_heads)
    rotated_key_rows = normalize_rotate(
        projected_key_heads, key_norm_gain, token_positions, kv_heads
    )
    query_grid = query_rows.reshape(seq_rows, kv_heads, head_groups, HEAD_WIDTH)
    score_scale = HEAD_WIDTH ** (-0.5)
    run_max = jnp.full((kv_heads, head_groups, seq_rows), NEG_LARGE, jnp.float32)
    key_piece = lax.all_gather(rotated_key_rows, "sp", axis=0, tiled=True).reshape(
        -1, kv_heads, HEAD_WIDTH
    )
    value_piece = lax.all_gather(projected_value_heads, "sp", axis=0, tiled=True).reshape(
        -1, kv_heads, HEAD_WIDTH
    )
    scores = (
        jnp.einsum("qhgd,khd->hgqk", query_grid, key_piece, preferred_element_type=jnp.float32)
        * score_scale
    )
    new_max = jnp.maximum(run_max, jnp.max(scores, axis=-1))
    weights = jnp.exp(scores - new_max[..., None])
    new_total = jnp.sum(weights, axis=-1)
    addition = jnp.einsum(
        "hgqk,khd->hgqd",
        weights.astype(jnp.bfloat16),
        value_piece,
        preferred_element_type=jnp.float32,
    )
    attended = (
        (addition / new_total[..., None])
        .transpose(2, 0, 1, 3)
        .reshape(seq_rows, q_heads * HEAD_WIDTH)
        .astype(jnp.bfloat16)
    )
    own_tokens = x_resid.shape[0]
    model_width = x_resid.shape[1]
    row_block = attended
    attn_proj = lax.psum_scatter(
        jnp.dot(row_block, out_weight, preferred_element_type=jnp.float32).astype(jnp.bfloat16),
        "tp",
        scatter_dimension=0,
        tiled=True,
    )
    middle = x_resid.astype(jnp.float32) + attn_proj.astype(jnp.float32)
    normed = rms_scale(middle, ffn_gain).astype(jnp.bfloat16)
    experts_all = lax.axis_size("sp") * expert_gate.shape[0]
    capacity = max(2, 2 * own_tokens * TOP // experts_all)
    flat_expert = routing.reshape(-1)
    one_hot = (flat_expert[:, None] == jnp.arange(experts_all, dtype=jnp.int32)[None, :]).astype(
        jnp.int32
    )
    earlier = jnp.cumsum(one_hot, axis=0) - one_hot
    slot_rank = jnp.sum(earlier * one_hot, axis=1)
    target = flat_expert * capacity + slot_rank
    chooser = (
        jnp.arange(experts_all * capacity, dtype=jnp.int32)[:, None] == target[None, :]
    ).astype(jnp.float32)
    gate_share = jax.nn.softmax(route_scores, axis=-1).reshape(-1)
    picker = jnp.sum(chooser.reshape(experts_all * capacity, own_tokens, TOP), axis=2).astype(
        jnp.bfloat16
    )
    combiner = jnp.sum(
        (chooser * gate_share[None, :]).reshape(experts_all * capacity, own_tokens, TOP), axis=2
    )
    dispatch = (
        jnp.dot(picker, normed, preferred_element_type=jnp.float32)
        .astype(jnp.bfloat16)
        .reshape(experts_all, capacity, model_width)
    )
    gate_matrix = expert_gate[0]
    up_matrix = expert_up[0]
    down_matrix = expert_down[0]
    arrived = lax.all_to_all(dispatch, "sp", split_axis=0, concat_axis=0, tiled=True)
    row_block = lax.all_gather(arrived.reshape(-1, model_width), "tp", axis=0, tiled=True)
    gate_part = jnp.dot(row_block, gate_matrix, preferred_element_type=jnp.float32)
    up_part = jnp.dot(row_block, up_matrix, preferred_element_type=jnp.float32)
    hidden = (jax.nn.silu(gate_part) * up_part).astype(jnp.bfloat16)
    row_block = hidden
    expert_result = lax.psum_scatter(
        jnp.dot(row_block, down_matrix, preferred_element_type=jnp.float32).astype(jnp.bfloat16),
        "tp",
        scatter_dimension=0,
        tiled=True,
    )
    returned = lax.all_to_all(
        expert_result.reshape(-1, capacity, model_width),
        "sp",
        split_axis=0,
        concat_axis=0,
        tiled=True,
    )
    routed = jnp.einsum(
        "st,sd->td",
        combiner,
        returned.reshape(-1, model_width).astype(jnp.float32),
        precision=lax.Precision.HIGHEST,
    )
    return (middle + routed).astype(jnp.bfloat16)


def rdma(src, dst, send_sem, recv_sem, device):
    return pltpu.make_async_remote_copy(
        src_ref=src,
        dst_ref=dst,
        send_sem=send_sem,
        recv_sem=recv_sem,
        device_id=device,
        device_id_type=MESH,
    )


def turn_head(values, gain, cosine, sine):
    values = values * lax.rsqrt(jnp.mean(values * values, axis=-1, keepdims=True) + NORM_EPS) * gain
    width = values.shape[1]
    quarter = width // 4
    lane = lax.broadcasted_iota(jnp.int32, values.shape, 1)
    swapped = jnp.where(
        lane % (2 * quarter) < quarter,
        pltpu.roll(values, width - quarter, 1),
        pltpu.roll(values, quarter, 1),
    )
    return (values * cosine + swapped * sine).astype(jnp.bfloat16)


def flip(index, mask):
    bit = 1
    while bit <= mask:
        if mask // bit % 2:
            index = index + bit * (1 - 2 * (index // bit % 2))
        bit = bit * 2
    return index


def hop_order(count):
    half, quarter = count // 2, count // 4
    near, far = list(range(half)), list(range(half, count))
    return near[:quarter] + far + near[quarter:]


def layer_kernel(
    n_sp,
    n_tp,
    capacity,
    q_ref,
    k_ref,
    v_ref,
    freq_ref,
    qg_ref,
    kg_ref,
    x_ref,
    fg_ref,
    route_ref,
    score_ref,
    ow_hbm,
    wg_hbm,
    wu_hbm,
    wd_hbm,
    out_ref,
    kbuf,
    vbuf,
    qs,
    att,
    part,
    rsbuf,
    mid,
    disp,
    rows,
    hid,
    eo,
    cor,
    pair,
    yrec,
    res,
    ret,
    ow,
    wg,
    wu,
    wd,
    w_sem,
    k_s,
    k_r,
    v_s,
    v_r,
    rs_s,
    rs_r,
    d_s,
    rows_r,
    y_s,
    c_s,
    e_s,
    e_r,
    p_s,
    p_r,
    b_s,
    b_r,
):
    s = lax.axis_index("sp")
    t = lax.axis_index("tp")
    n_x = math.isqrt(n_sp // 2)
    if n_x == 0 or n_sp % n_x:
        n_x = 1
    n_z = n_sp // n_x
    n_y = n_tp // 2
    y, c = t // 2, t % 2
    core_peer = (s, y * 2 + 1 - c)
    order = hop_order(n_sp)
    seq_rows, q_width = q_ref.shape
    kv_width = k_ref.shape[1]
    q_heads, kv_heads = q_width // HEAD_WIDTH, kv_width // HEAD_WIDTH
    groups = q_heads // kv_heads
    own, model = x_ref.shape
    f_width = wg.shape[1]
    pending = []

    def send(src, dst, send_sem, recv_sem, device):
        copy = rdma(src, dst, send_sem, recv_sem, device)
        copy.start()
        pending.append(copy)

    def arrive(dst, recv_sem):
        rdma(dst, dst, recv_sem, recv_sem, core_peer).wait_recv()

    weight_copies = [
        pltpu.make_async_copy(ow_hbm, ow, w_sem.at[0]),
        pltpu.make_async_copy(wg_hbm.at[0], wg, w_sem.at[1]),
        pltpu.make_async_copy(wu_hbm.at[0], wu, w_sem.at[2]),
        pltpu.make_async_copy(wd_hbm.at[0], wd, w_sem.at[3]),
    ]
    for copy in weight_copies:
        copy.start()

    barrier = pltpu.get_barrier_semaphore()
    for d in range(1, n_sp):
        pl.semaphore_signal(barrier, inc=1, device_id=((s + d) % n_sp, t), device_id_type=MESH)
    for d in range(1, n_tp):
        pl.semaphore_signal(barrier, inc=1, device_id=(s, (t + d) % n_tp), device_id_type=MESH)

    table = (seq_rows, HEAD_WIDTH)
    place = lax.broadcasted_iota(jnp.int32, table, 0) + s * seq_rows
    column = lax.broadcasted_iota(jnp.int32, table, 1)
    step = jnp.where(column < HEAD_WIDTH // 2, place // GRID_W, place % GRID_W)
    angles = step.astype(jnp.float32) * freq_ref[...]
    cosine, sine = jnp.cos(angles), jnp.sin(angles)
    sine = jnp.where(column % (HEAD_WIDTH // 2) < HEAD_WIDTH // 4, -sine, sine)
    for h in range(kv_heads):
        cols = slice(h * HEAD_WIDTH, (h + 1) * HEAD_WIDTH)
        kbuf[0, :, cols] = turn_head(k_ref[:, cols].astype(jnp.float32), kg_ref[...], cosine, sine)
    pl.semaphore_wait(barrier, n_sp - 1 + n_tp - 1)

    for buf, first, s_sem, r_sem in ((kbuf, kbuf.at[0], k_s, k_r), (vbuf, v_ref, v_s, v_r)):
        for slot in list(range(1, n_x)) + list(range(n_x, n_sp, n_x)):
            send(first, buf.at[slot], s_sem.at[slot], r_sem.at[slot], (flip(s, slot), t))
    vbuf[0] = v_ref[...]
    for h in range(q_heads):
        cols = slice(h * HEAD_WIDTH, (h + 1) * HEAD_WIDTH)
        kv, member = h // groups, h % groups
        qs[kv, member * seq_rows : (member + 1) * seq_rows, :] = turn_head(
            q_ref[:, cols].astype(jnp.float32), qg_ref[...], cosine, sine
        )
    total_slots = n_sp * capacity
    slot_at = lax.broadcasted_iota(jnp.int32, (total_slots, own), 0)
    slot_place = slot_at // capacity
    slot_expert = jnp.zeros_like(slot_at)
    for k, d in enumerate(order):
        slot_expert = jnp.where(slot_place == k, flip(s, d), slot_expert)
    first_hit = route_ref[0:1, :] == slot_expert
    named = first_hit | (route_ref[1:2, :] == slot_expert)
    earlier = (
        lax.broadcasted_iota(jnp.int32, (own, own), 0)
        < lax.broadcasted_iota(jnp.int32, (own, own), 1)
    )
    rank = jnp.dot(
        named.astype(jnp.float32).astype(jnp.bfloat16),
        earlier.astype(jnp.float32).astype(jnp.bfloat16),
        preferred_element_type=jnp.float32,
    )
    picked = jnp.where(
        named & (rank == (slot_at % capacity).astype(jnp.float32)), 1.0, 0.0
    )
    route_scores = score_ref[...]
    share = jnp.exp(route_scores - jnp.max(route_scores, axis=0, keepdims=True))
    share = share / jnp.sum(share, axis=0, keepdims=True)
    combiner = picked * jnp.where(first_hit, share[0:1, :], share[1:2, :])
    picker = picked.astype(jnp.bfloat16)

    for buf, s_sem, r_sem in ((kbuf, k_s, k_r), (vbuf, v_s, v_r)):
        for dz in range(1, n_z):
            slot = dz * n_x
            arrive(buf.at[slot], r_sem.at[slot])
            for dx in range(1, n_x):
                send(
                    buf.at[slot],
                    buf.at[slot + dx],
                    s_sem.at[slot + dx],
                    r_sem.at[slot + dx],
                    (flip(s, dx), t),
                )
    for slot in range(n_sp):
        if slot % n_x:
            arrive(kbuf.at[slot], k_r.at[slot])
    keys_all = n_sp * seq_rows
    score_scale = HEAD_WIDTH ** (-0.5)
    heads_done = []
    for kv in range(kv_heads):
        cols = slice(kv * HEAD_WIDTH, (kv + 1) * HEAD_WIDTH)
        keys = kbuf[:, :, cols].reshape(keys_all, HEAD_WIDTH)
        scores = (
            lax.dot_general(
                qs[kv], keys, (((1,), (1,)), ((), ())), preferred_element_type=jnp.float32
            )
            * score_scale
        )
        weights = jnp.exp(scores - jnp.max(scores, axis=-1, keepdims=True))
        total = jnp.sum(weights, axis=-1, keepdims=True)
        heads_done.append((weights.astype(jnp.bfloat16), total))
    for slot in range(n_sp):
        if slot % n_x:
            arrive(vbuf.at[slot], v_r.at[slot])
    for kv in range(kv_heads):
        cols = slice(kv * HEAD_WIDTH, (kv + 1) * HEAD_WIDTH)
        values = vbuf[:, :, cols].reshape(keys_all, HEAD_WIDTH)
        weights, total = heads_done[kv]
        mixed = jnp.dot(weights, values, preferred_element_type=jnp.float32) / total
        for member in range(groups):
            h = kv * groups + member
            att[:, h * HEAD_WIDTH : (h + 1) * HEAD_WIDTH] = mixed[
                member * seq_rows : (member + 1) * seq_rows
            ].astype(jnp.bfloat16)

    weight_copies[0].wait()
    tile = min(512, model)
    for j in range(model // tile):
        cols = slice(j * tile, (j + 1) * tile)
        part[:, :, cols] = (
            jnp.dot(att[...], ow[:, cols], preferred_element_type=jnp.float32)
            .astype(jnp.bfloat16)
            .reshape(n_tp, own, tile)
        )
    for d in range(n_tp - 1, 0, -1):
        peer = flip(t, d)
        send(part.at[peer], rsbuf.at[d], rs_s.at[d], rs_r.at[d], (s, peer))
    summed = part[t].astype(jnp.float32)
    for d in range(1, n_tp):
        arrive(rsbuf.at[d], rs_r.at[d])
        summed = summed + rsbuf[d].astype(jnp.float32)
    middle = x_ref[...].astype(jnp.float32) + summed.astype(jnp.bfloat16).astype(jnp.float32)
    mid[...] = middle
    normed = (
        middle
        * lax.rsqrt(jnp.mean(middle * middle, axis=-1, keepdims=True) + NORM_EPS)
        * fg_ref[...]
    ).astype(jnp.bfloat16)
    chosen = (
        jnp.dot(picker, normed, preferred_element_type=jnp.float32)
        .astype(jnp.bfloat16)
        .reshape(n_sp, capacity, model)
    )
    disp[...] = chosen
    for k, d in enumerate(order):
        if k:
            send(disp.at[k], rows.at[k, t], d_s.at[k], rows_r.at[k, t], (flip(s, d), t))
    rows[0, t] = chosen[0]

    def forward(k):
        if k:
            arrive(rows.at[k, t], rows_r.at[k, t])
        for dy in range(1, n_y):
            peer = ((y + dy) % n_y) * 2 + c
            send(rows.at[k, t], rows.at[k, t], y_s.at[k, dy], rows_r.at[k, t], (s, peer))
        send(rows.at[k, t], rows.at[k, t], c_s.at[k, 0], rows_r.at[k, t], core_peer)

    def relay(k):
        for dy in range(1, n_y):
            source = ((y + n_y - dy) % n_y) * 2 + c
            arrive(rows.at[k, source], rows_r.at[k, source])
            send(
                rows.at[k, source],
                rows.at[k, source],
                c_s.at[k, dy],
                rows_r.at[k, source],
                core_peer,
            )

    def settle(k):
        for dy in range(n_y):
            source = ((y + n_y - dy) % n_y) * 2 + 1 - c
            arrive(rows.at[k, source], rows_r.at[k, source])

    n_groups = 2
    group = n_sp // n_groups
    group_rows = group * n_tp * capacity

    def give_pair(g):
        ks = pl.ds(g * group, group)
        send(eo.at[1 - c, :, ks], cor.at[:, ks], e_s.at[g], e_r.at[g], core_peer)

    def sum_pair(g):
        arrive(cor.at[:, pl.ds(g * group, group)], e_r.at[g])
        for k in range(group - 1, -1, -1) if g == 0 else range(group, n_sp):
            for dy in range(1, n_y):
                far = (y + dy) % n_y
                pair[dy, k] = (
                    eo[c, far, k].astype(jnp.float32) + cor[far, k].astype(jnp.float32)
                ).astype(jnp.bfloat16)
                send(
                    pair.at[dy, k], yrec.at[dy, k], p_s.at[k, dy], p_r.at[k, dy], (s, far * 2 + c)
                )

    def give_back(k):
        whole = eo[c, y, k].astype(jnp.float32) + cor[y, k].astype(jnp.float32)
        for dy in range(1, n_y):
            arrive(yrec.at[dy, k], p_r.at[k, dy])
            whole = whole + yrec[dy, k].astype(jnp.float32)
        if k == 0:
            ret[0] = whole.astype(jnp.bfloat16)
        else:
            res[k] = whole.astype(jnp.bfloat16)
            send(res.at[k], ret.at[k], b_s.at[k], b_r.at[k], (flip(s, order[k]), t))

    def experts(g, hooks):
        hooks = list(hooks)
        block = rows[g * group : (g + 1) * group].reshape(group_rows, model)
        f_tile = min(256, f_width)
        for j in range(f_width // f_tile):
            cols = slice(j * f_tile, (j + 1) * f_tile)
            gate = jnp.dot(block, wg[:, cols], preferred_element_type=jnp.float32)
            up = jnp.dot(block, wu[:, cols], preferred_element_type=jnp.float32)
            hid[:, cols] = (gate / (1.0 + jnp.exp(-gate)) * up).astype(jnp.bfloat16)
            if hooks:
                hooks.pop(0)()
        if g == 0:
            weight_copies[3].wait()
        for j in range(model // tile):
            cols = slice(j * tile, (j + 1) * tile)
            down = jnp.dot(hid[...], wd[:, cols], preferred_element_type=jnp.float32)
            down = down.astype(jnp.bfloat16).reshape(group, n_y, 2, capacity, tile)
            for core in range(2):
                for far in range(n_y):
                    eo[core, far, g * group : (g + 1) * group, :, cols] = down[:, far, core]
            if hooks:
                hooks.pop(0)()
        for hook in hooks:
            hook()

    for k in range(group):
        forward(k)
    for k in range(group):
        relay(k)
    for k in range(group):
        settle(k)
    weight_copies[1].wait()
    weight_copies[2].wait()
    late = range(group, n_sp)
    experts(
        0,
        [functools.partial(forward, k) for k in late] + [functools.partial(relay, k) for k in late],
    )
    give_pair(0)
    for k in late:
        settle(k)
    nothing = lambda: None
    early = [functools.partial(give_back, k) for k in (*range(group - 1, -1, -1),)]
    experts(1, [functools.partial(sum_pair, 0), nothing, nothing] + early)
    give_pair(1)
    sum_pair(1)
    for k in late:
        give_back(k)
    for k in range(1, n_sp):
        arrive(ret.at[k], b_r.at[k])
    high = combiner.astype(jnp.bfloat16)
    rest = combiner - high.astype(jnp.float32)
    middle_part = rest.astype(jnp.bfloat16)
    low = (rest - middle_part.astype(jnp.float32)).astype(jnp.bfloat16)
    returned = ret[...].reshape(total_slots, model)
    routed = jnp.zeros((own, model), jnp.float32)
    for piece in (high, middle_part, low):
        routed = routed + lax.dot_general(
            piece, returned, (((0,), (0,)), ((), ())), preferred_element_type=jnp.float32
        )
    out_ref[...] = mid[...] + routed
    for copy in pending:
        copy.wait_send()


def head_frequency():
    quarter = HEAD_WIDTH // 4
    frequency = ROPE_BASE ** (-np.arange(quarter, dtype=np.float32) / quarter)
    return jnp.asarray(np.tile(frequency, 4).reshape(1, HEAD_WIDTH), jnp.float32)


def local(
    x_resid,
    query_proj,
    projected_key_heads,
    projected_value_heads,
    query_gain,
    key_norm_gain,
    out_weight,
    ffn_gain,
    routing,
    route_scores,
    expert_gate,
    expert_up,
    expert_down,
):
    n_sp, n_tp = lax.axis_size("sp"), lax.axis_size("tp")
    own, model = x_resid.shape
    experts_all = n_sp * expert_gate.shape[0]
    capacity = max(2, 2 * own * TOP // experts_all)
    if capacity % 16 or n_tp & (n_tp - 1) or n_sp & (n_sp - 1) or n_tp < 2 or n_sp < 4 or expert_gate.shape[0] != 1:
        return local_plain(
            x_resid,
            query_proj,
            projected_key_heads,
            projected_value_heads,
            query_gain,
            key_norm_gain,
            out_weight,
            ffn_gain,
            routing,
            route_scores,
            expert_gate,
            expert_up,
            expert_down,
        )
    seq_rows, q_width = query_proj.shape
    kv_width = projected_key_heads.shape[1]
    kv_heads = kv_width // HEAD_WIDTH
    groups = q_width // kv_width
    f_width = expert_gate.shape[2]
    n_y = n_tp // 2
    bf16 = jnp.bfloat16
    dma = pltpu.SemaphoreType.DMA
    vmem = pl.BlockSpec(memory_space=pltpu.VMEM)
    hbm = pl.BlockSpec(memory_space=pl.ANY)
    return pl.pallas_call(
        functools.partial(layer_kernel, n_sp, n_tp, capacity),
        out_shape=jax.ShapeDtypeStruct((own, model), jnp.float32),
        in_specs=[vmem] * 10 + [hbm] * 4,
        out_specs=vmem,
        scratch_shapes=[
            pltpu.VMEM((n_sp, seq_rows, kv_width), bf16),
            pltpu.VMEM((n_sp, seq_rows, kv_width), bf16),
            pltpu.VMEM((kv_heads, groups * seq_rows, HEAD_WIDTH), bf16),
            pltpu.VMEM((seq_rows, q_width), bf16),
            pltpu.VMEM((n_tp, own, model), bf16),
            pltpu.VMEM((n_tp, own, model), bf16),
            pltpu.VMEM((own, model), jnp.float32),
            pltpu.VMEM((n_sp, capacity, model), bf16),
            pltpu.VMEM((n_sp, n_tp, capacity, model), bf16),
            pltpu.VMEM((n_sp // 2 * n_tp * capacity, f_width), bf16),
            pltpu.VMEM((2, n_y, n_sp, capacity, model), bf16),
            pltpu.VMEM((n_y, n_sp, capacity, model), bf16),
            pltpu.VMEM((n_y, n_sp, capacity, model), bf16),
            pltpu.VMEM((n_y, n_sp, capacity, model), bf16),
            pltpu.VMEM((n_sp, capacity, model), bf16),
            pltpu.VMEM((n_sp, capacity, model), bf16),
            pltpu.VMEM(out_weight.shape, bf16),
            pltpu.VMEM(expert_gate.shape[1:], bf16),
            pltpu.VMEM(expert_up.shape[1:], bf16),
            pltpu.VMEM(expert_down.shape[1:], bf16),
            dma((4,)),
            dma((n_sp,)),
            dma((n_sp,)),
            dma((n_sp,)),
            dma((n_sp,)),
            dma((n_tp,)),
            dma((n_tp,)),
            dma((n_sp,)),
            dma((n_sp, n_tp)),
            dma((n_sp, n_y)),
            dma((n_sp, n_y)),
            dma((2,)),
            dma((2,)),
            dma((n_sp, n_y)),
            dma((n_sp, n_y)),
            dma((n_sp,)),
            dma((n_sp,)),
        ],
        compiler_params=pltpu.CompilerParams(
            collective_id=0, has_side_effects=True, vmem_limit_bytes=56 * 1024 * 1024
        ),
    )(
        query_proj,
        projected_key_heads,
        projected_value_heads,
        head_frequency(),
        query_gain.reshape(1, -1),
        key_norm_gain.reshape(1, -1),
        x_resid,
        ffn_gain.reshape(1, -1),
        routing.T,
        route_scores.T,
        out_weight,
        expert_gate,
        expert_up,
        expert_down,
    ).astype(bf16)


def solution(mesh):
    in_specs = (
        P(("sp", "tp"), None),
        P("sp", "tp"),
        P("sp", "tp"),
        P("sp", "tp"),
        P(),
        P(),
        P("tp", None),
        P(),
        P(("sp", "tp"), None),
        P(("sp", "tp"), None),
        P("sp", None, "tp"),
        P("sp", None, "tp"),
        P("sp", "tp", None),
    )
    out_specs = P(("sp", "tp"), None)
    return jax.shard_map(local, mesh=mesh, in_specs=in_specs, out_specs=out_specs, check_vma=False)
```

```python
import functools
import math

import jax
import jax.numpy as jnp
import numpy as np
from jax import lax
from jax.experimental import pallas as pl
from jax.experimental.pallas import tpu as pltpu
from jax.sharding import PartitionSpec as P

MESH = pl.DeviceIdType.MESH

HEAD_WIDTH = 128
TOP = 2
GRID_W = 64


NORM_EPS = 1e-06
ROPE_BASE = 10000.0
NEG_LARGE = -1e30


def rms_scale(values, norm_gain):
    return (
        values * lax.rsqrt(jnp.mean(values * values, axis=-1, keepdims=True) + NORM_EPS) * norm_gain
    )


def grid_angles(token_positions, head_size):
    freq_count = head_size // 4
    frequency = ROPE_BASE ** (-jnp.arange(freq_count, dtype=jnp.float32) / freq_count)
    grid_row = (token_positions // GRID_W).astype(jnp.float32)
    grid_col = (token_positions % GRID_W).astype(jnp.float32)
    return (grid_row[:, None] * frequency, grid_col[:, None] * frequency)


def turn_half(values, angles):
    cosine = jnp.cos(angles)[:, None, :]
    sine_part = jnp.sin(angles)[:, None, :]
    leading, trailing = jnp.split(values, 2, axis=-1)
    return jnp.concatenate(
        [leading * cosine - trailing * sine_part, trailing * cosine + leading * sine_part], axis=-1
    )


def normalize_rotate(projected, norm_gain, token_positions, heads):
    length = projected.shape[0]
    values = projected.astype(jnp.float32).reshape(length, heads, -1)
    head_size = values.shape[-1]
    values = rms_scale(values, norm_gain)
    row_angle, col_angle = grid_angles(token_positions, head_size)
    half_size = head_size // 2
    turned = jnp.concatenate(
        [
            turn_half(values[..., :half_size], row_angle),
            turn_half(values[..., half_size:], col_angle),
        ],
        axis=-1,
    )
    return turned.reshape(length, heads * head_size).astype(jnp.bfloat16)


def local_plain(
    x_resid,
    query_proj,
    projected_key_heads,
    projected_value_heads,
    query_gain,
    key_norm_gain,
    out_weight,
    ffn_gain,
    routing,
    route_scores,
    expert_gate,
    expert_up,
    expert_down,
):
    seq_rows = query_proj.shape[0]
    q_heads = query_proj.shape[1] // HEAD_WIDTH
    kv_heads = projected_key_heads.shape[1] // HEAD_WIDTH
    head_groups = q_heads // kv_heads
    token_positions = lax.axis_index("sp") * seq_rows + jnp.arange(seq_rows, dtype=jnp.int32)
    query_rows = normalize_rotate(query_proj, query_gain, token_positions, q_heads)
    rotated_key_rows = normalize_rotate(
        projected_key_heads, key_norm_gain, token_positions, kv_heads
    )
    query_grid = query_rows.reshape(seq_rows, kv_heads, head_groups, HEAD_WIDTH)
    score_scale = HEAD_WIDTH ** (-0.5)
    run_max = jnp.full((kv_heads, head_groups, seq_rows), NEG_LARGE, jnp.float32)
    key_piece = lax.all_gather(rotated_key_rows, "sp", axis=0, tiled=True).reshape(
        -1, kv_heads, HEAD_WIDTH
    )
    value_piece = lax.all_gather(projected_value_heads, "sp", axis=0, tiled=True).reshape(
        -1, kv_heads, HEAD_WIDTH
    )
    scores = (
        jnp.einsum("qhgd,khd->hgqk", query_grid, key_piece, preferred_element_type=jnp.float32)
        * score_scale
    )
    new_max = jnp.maximum(run_max, jnp.max(scores, axis=-1))
    weights = jnp.exp(scores - new_max[..., None])
    new_total = jnp.sum(weights, axis=-1)
    addition = jnp.einsum(
        "hgqk,khd->hgqd",
        weights.astype(jnp.bfloat16),
        value_piece,
        preferred_element_type=jnp.float32,
    )
    attended = (
        (addition / new_total[..., None])
        .transpose(2, 0, 1, 3)
        .reshape(seq_rows, q_heads * HEAD_WIDTH)
        .astype(jnp.bfloat16)
    )
    own_tokens = x_resid.shape[0]
    model_width = x_resid.shape[1]
    row_block = attended
    attn_proj = lax.psum_scatter(
        jnp.dot(row_block, out_weight, preferred_element_type=jnp.float32).astype(jnp.bfloat16),
        "tp",
        scatter_dimension=0,
        tiled=True,
    )
    middle = x_resid.astype(jnp.float32) + attn_proj.astype(jnp.float32)
    normed = rms_scale(middle, ffn_gain).astype(jnp.bfloat16)
    experts_all = lax.axis_size("sp") * expert_gate.shape[0]
    capacity = max(2, 2 * own_tokens * TOP // experts_all)
    flat_expert = routing.reshape(-1)
    one_hot = (flat_expert[:, None] == jnp.arange(experts_all, dtype=jnp.int32)[None, :]).astype(
        jnp.int32
    )
    earlier = jnp.cumsum(one_hot, axis=0) - one_hot
    slot_rank = jnp.sum(earlier * one_hot, axis=1)
    target = flat_expert * capacity + slot_rank
    chooser = (
        jnp.arange(experts_all * capacity, dtype=jnp.int32)[:, None] == target[None, :]
    ).astype(jnp.float32)
    gate_share = jax.nn.softmax(route_scores, axis=-1).reshape(-1)
    picker = jnp.sum(chooser.reshape(experts_all * capacity, own_tokens, TOP), axis=2).astype(
        jnp.bfloat16
    )
    combiner = jnp.sum(
        (chooser * gate_share[None, :]).reshape(experts_all * capacity, own_tokens, TOP), axis=2
    )
    dispatch = (
        jnp.dot(picker, normed, preferred_element_type=jnp.float32)
        .astype(jnp.bfloat16)
        .reshape(experts_all, capacity, model_width)
    )
    gate_matrix = expert_gate[0]
    up_matrix = expert_up[0]
    down_matrix = expert_down[0]
    arrived = lax.all_to_all(dispatch, "sp", split_axis=0, concat_axis=0, tiled=True)
    row_block = lax.all_gather(arrived.reshape(-1, model_width), "tp", axis=0, tiled=True)
    gate_part = jnp.dot(row_block, gate_matrix, preferred_element_type=jnp.float32)
    up_part = jnp.dot(row_block, up_matrix, preferred_element_type=jnp.float32)
    hidden = (jax.nn.silu(gate_part) * up_part).astype(jnp.bfloat16)
    row_block = hidden
    expert_result = lax.psum_scatter(
        jnp.dot(row_block, down_matrix, preferred_element_type=jnp.float32).astype(jnp.bfloat16),
        "tp",
        scatter_dimension=0,
        tiled=True,
    )
    returned = lax.all_to_all(
        expert_result.reshape(-1, capacity, model_width),
        "sp",
        split_axis=0,
        concat_axis=0,
        tiled=True,
    )
    routed = jnp.einsum(
        "st,sd->td",
        combiner,
        returned.reshape(-1, model_width).astype(jnp.float32),
        precision=lax.Precision.HIGHEST,
    )
    return (middle + routed).astype(jnp.bfloat16)


def rdma(src, dst, send_sem, recv_sem, device):
    return pltpu.make_async_remote_copy(
        src_ref=src,
        dst_ref=dst,
        send_sem=send_sem,
        recv_sem=recv_sem,
        device_id=device,
        device_id_type=MESH,
    )


def turn_head(values, gain, cosine, sine):
    values = values * lax.rsqrt(jnp.mean(values * values, axis=-1, keepdims=True) + NORM_EPS) * gain
    width = values.shape[1]
    quarter = width // 4
    lane = lax.broadcasted_iota(jnp.int32, values.shape, 1)
    swapped = jnp.where(
        lane % (2 * quarter) < quarter,
        pltpu.roll(values, width - quarter, 1),
        pltpu.roll(values, quarter, 1),
    )
    return (values * cosine + swapped * sine).astype(jnp.bfloat16)


def flip(index, mask):
    bit = 1
    while bit <= mask:
        if mask // bit % 2:
            index = index + bit * (1 - 2 * (index // bit % 2))
        bit = bit * 2
    return index


def hop_order(count):
    half, quarter = count // 2, count // 4
    near, far = list(range(half)), list(range(half, count))
    return near[:quarter] + far + near[quarter:]


def layer_kernel(
    n_sp,
    n_tp,
    capacity,
    q_ref,
    k_ref,
    v_ref,
    freq_ref,
    qg_ref,
    kg_ref,
    x_ref,
    fg_ref,
    route_ref,
    score_ref,
    ow_hbm,
    wg_hbm,
    wu_hbm,
    wd_hbm,
    out_ref,
    kbuf,
    vbuf,
    qs,
    att,
    part,
    rsbuf,
    mid,
    disp,
    rows,
    hid,
    eo,
    cor,
    pair,
    yrec,
    res,
    ret,
    ow,
    wg,
    wu,
    wd,
    w_sem,
    k_s,
    k_r,
    v_s,
    v_r,
    rs_s,
    rs_r,
    d_s,
    rows_r,
    y_s,
    c_s,
    e_s,
    e_r,
    p_s,
    p_r,
    b_s,
    b_r,
):
    s = lax.axis_index("sp")
    t = lax.axis_index("tp")
    n_x = math.isqrt(n_sp // 2)
    if n_x == 0 or n_sp % n_x:
        n_x = 1
    n_z = n_sp // n_x
    n_y = n_tp // 2
    y, c = t // 2, t % 2
    core_peer = (s, y * 2 + 1 - c)
    order = hop_order(n_sp)
    seq_rows, q_width = q_ref.shape
    kv_width = k_ref.shape[1]
    q_heads, kv_heads = q_width // HEAD_WIDTH, kv_width // HEAD_WIDTH
    groups = q_heads // kv_heads
    own, model = x_ref.shape
    f_width = wg.shape[1]
    pending = []

    def send(src, dst, send_sem, recv_sem, device):
        copy = rdma(src, dst, send_sem, recv_sem, device)
        copy.start()
        pending.append(copy)

    def arrive(dst, recv_sem):
        rdma(dst, dst, recv_sem, recv_sem, core_peer).wait_recv()

    weight_copies = [
        pltpu.make_async_copy(ow_hbm, ow, w_sem.at[0]),
        pltpu.make_async_copy(wg_hbm.at[0], wg, w_sem.at[1]),
        pltpu.make_async_copy(wu_hbm.at[0], wu, w_sem.at[2]),
        pltpu.make_async_copy(wd_hbm.at[0], wd, w_sem.at[3]),
    ]
    for copy in weight_copies:
        copy.start()

    barrier = pltpu.get_barrier_semaphore()
    for d in range(1, n_sp):
        pl.semaphore_signal(barrier, inc=1, device_id=((s + d) % n_sp, t), device_id_type=MESH)
    for d in range(1, n_tp):
        pl.semaphore_signal(barrier, inc=1, device_id=(s, (t + d) % n_tp), device_id_type=MESH)

    table = (seq_rows, HEAD_WIDTH)
    place = lax.broadcasted_iota(jnp.int32, table, 0) + s * seq_rows
    column = lax.broadcasted_iota(jnp.int32, table, 1)
    step = jnp.where(column < HEAD_WIDTH // 2, place // GRID_W, place % GRID_W)
    angles = step.astype(jnp.float32) * freq_ref[...]
    cosine, sine = jnp.cos(angles), jnp.sin(angles)
    sine = jnp.where(column % (HEAD_WIDTH // 2) < HEAD_WIDTH // 4, -sine, sine)
    for h in range(kv_heads):
        cols = slice(h * HEAD_WIDTH, (h + 1) * HEAD_WIDTH)
        kbuf[0, :, cols] = turn_head(k_ref[:, cols].astype(jnp.float32), kg_ref[...], cosine, sine)
    pl.semaphore_wait(barrier, n_sp - 1 + n_tp - 1)

    for slot in list(range(1, n_x)) + list(range(n_x, n_sp, n_x)):
        send(kbuf.at[0], kbuf.at[slot], k_s.at[slot], k_r.at[slot], (flip(s, slot), t))

    def send_values(slot):
        send(v_ref, vbuf.at[slot], v_s.at[slot], v_r.at[slot], (flip(s, slot), t))

    for slot in range(1, n_x):
        send_values(slot)
    vbuf[0] = v_ref[...]
    for h in range(q_heads):
        cols = slice(h * HEAD_WIDTH, (h + 1) * HEAD_WIDTH)
        kv, member = h // groups, h % groups
        qs[kv, member * seq_rows : (member + 1) * seq_rows, :] = turn_head(
            q_ref[:, cols].astype(jnp.float32), qg_ref[...], cosine, sine
        )
    total_slots = n_sp * capacity
    slot_at = lax.broadcasted_iota(jnp.int32, (total_slots, own), 0)
    slot_place = slot_at // capacity
    slot_expert = jnp.zeros_like(slot_at)
    for k, d in enumerate(order):
        slot_expert = jnp.where(slot_place == k, flip(s, d), slot_expert)
    first_hit = route_ref[0:1, :] == slot_expert
    named = first_hit | (route_ref[1:2, :] == slot_expert)
    earlier = (
        lax.broadcasted_iota(jnp.int32, (own, own), 0)
        < lax.broadcasted_iota(jnp.int32, (own, own), 1)
    )
    rank = jnp.dot(
        named.astype(jnp.float32).astype(jnp.bfloat16),
        earlier.astype(jnp.float32).astype(jnp.bfloat16),
        preferred_element_type=jnp.float32,
    )
    picked = jnp.where(
        named & (rank == (slot_at % capacity).astype(jnp.float32)), 1.0, 0.0
    )
    route_scores = score_ref[...]
    share = jnp.exp(route_scores - jnp.max(route_scores, axis=0, keepdims=True))
    share = share / jnp.sum(share, axis=0, keepdims=True)
    combiner = picked * jnp.where(first_hit, share[0:1, :], share[1:2, :])
    picker = picked.astype(jnp.bfloat16)

    for buf, s_sem, r_sem in ((kbuf, k_s, k_r), (vbuf, v_s, v_r)):
        for dz in range(1, n_z):
            slot = dz * n_x
            arrive(buf.at[slot], r_sem.at[slot])
            for dx in range(1, n_x):
                send(
                    buf.at[slot],
                    buf.at[slot + dx],
                    s_sem.at[slot + dx],
                    r_sem.at[slot + dx],
                    (flip(s, dx), t),
                )
            if buf is kbuf:
                send_values(slot)
    for slot in range(n_sp):
        if slot % n_x:
            arrive(kbuf.at[slot], k_r.at[slot])
    keys_all = n_sp * seq_rows
    score_scale = HEAD_WIDTH ** (-0.5)
    heads_done = []
    for kv in range(kv_heads):
        cols = slice(kv * HEAD_WIDTH, (kv + 1) * HEAD_WIDTH)
        keys = kbuf[:, :, cols].reshape(keys_all, HEAD_WIDTH)
        scores = (
            lax.dot_general(
                qs[kv], keys, (((1,), (1,)), ((), ())), preferred_element_type=jnp.float32
            )
            * score_scale
        )
        weights = jnp.exp(scores - jnp.max(scores, axis=-1, keepdims=True))
        total = jnp.sum(weights, axis=-1, keepdims=True)
        heads_done.append((weights.astype(jnp.bfloat16), total))
    for slot in range(n_sp):
        if slot % n_x:
            arrive(vbuf.at[slot], v_r.at[slot])
    for kv in range(kv_heads):
        cols = slice(kv * HEAD_WIDTH, (kv + 1) * HEAD_WIDTH)
        values = vbuf[:, :, cols].reshape(keys_all, HEAD_WIDTH)
        weights, total = heads_done[kv]
        mixed = jnp.dot(weights, values, preferred_element_type=jnp.float32) / total
        for member in range(groups):
            h = kv * groups + member
            att[:, h * HEAD_WIDTH : (h + 1) * HEAD_WIDTH] = mixed[
                member * seq_rows : (member + 1) * seq_rows
            ].astype(jnp.bfloat16)

    weight_copies[0].wait()
    tile = min(512, model)
    for j in range(model // tile):
        cols = slice(j * tile, (j + 1) * tile)
        part[:, :, cols] = (
            jnp.dot(att[...], ow[:, cols], preferred_element_type=jnp.float32)
            .astype(jnp.bfloat16)
            .reshape(n_tp, own, tile)
        )
    for d in range(n_tp - 1, 0, -1):
        peer = flip(t, d)
        send(part.at[peer], rsbuf.at[d], rs_s.at[d], rs_r.at[d], (s, peer))
    summed = part[t].astype(jnp.float32)
    for d in range(1, n_tp):
        arrive(rsbuf.at[d], rs_r.at[d])
        summed = summed + rsbuf[d].astype(jnp.float32)
    middle = x_ref[...].astype(jnp.float32) + summed.astype(jnp.bfloat16).astype(jnp.float32)
    mid[...] = middle
    normed = (
        middle
        * lax.rsqrt(jnp.mean(middle * middle, axis=-1, keepdims=True) + NORM_EPS)
        * fg_ref[...]
    ).astype(jnp.bfloat16)
    chosen = (
        jnp.dot(picker, normed, preferred_element_type=jnp.float32)
        .astype(jnp.bfloat16)
        .reshape(n_sp, capacity, model)
    )
    disp[...] = chosen

    def dispatch(k):
        send(disp.at[k], rows.at[k, t], d_s.at[k], rows_r.at[k, t], (flip(s, order[k]), t))

    window = n_sp // 2
    for k in range(1, window):
        dispatch(k)
    rows[0, t] = chosen[0]

    def forward(k):
        if k:
            arrive(rows.at[k, t], rows_r.at[k, t])
        for dy in range(1, n_y):
            peer = ((y + dy) % n_y) * 2 + c
            send(rows.at[k, t], rows.at[k, t], y_s.at[k, dy], rows_r.at[k, t], (s, peer))
        send(rows.at[k, t], rows.at[k, t], c_s.at[k, 0], rows_r.at[k, t], core_peer)

    def relay(k):
        for dy in range(1, n_y):
            source = ((y + n_y - dy) % n_y) * 2 + c
            arrive(rows.at[k, source], rows_r.at[k, source])
            send(
                rows.at[k, source],
                rows.at[k, source],
                c_s.at[k, dy],
                rows_r.at[k, source],
                core_peer,
            )

    def settle(k):
        for dy in range(n_y):
            source = ((y + n_y - dy) % n_y) * 2 + 1 - c
            arrive(rows.at[k, source], rows_r.at[k, source])

    n_groups = 2
    group = n_sp // n_groups
    group_rows = group * n_tp * capacity

    def give_pair(g):
        ks = pl.ds(g * group, group)
        send(eo.at[1 - c, :, ks], cor.at[:, ks], e_s.at[g], e_r.at[g], core_peer)

    def sum_pair(k):
        for dy in range(1, n_y):
            far = (y + dy) % n_y
            pair[dy, k] = (
                eo[c, far, k].astype(jnp.float32) + cor[far, k].astype(jnp.float32)
            ).astype(jnp.bfloat16)
            send(pair.at[dy, k], yrec.at[dy, k], p_s.at[k, dy], p_r.at[k, dy], (s, far * 2 + c))

    def start_pairs(g, slots):
        arrive(cor.at[:, pl.ds(g * group, group)], e_r.at[g])
        for k in slots[:2]:
            sum_pair(k)

    def return_next(i, slots):
        give_back(slots[i])
        if i + 2 < len(slots):
            sum_pair(slots[i + 2])

    def give_back(k):
        whole = eo[c, y, k].astype(jnp.float32) + cor[y, k].astype(jnp.float32)
        for dy in range(1, n_y):
            arrive(yrec.at[dy, k], p_r.at[k, dy])
            whole = whole + yrec[dy, k].astype(jnp.float32)
        if k == 0:
            ret[0] = whole.astype(jnp.bfloat16)
        else:
            res[k] = whole.astype(jnp.bfloat16)
            send(res.at[k], ret.at[k], b_s.at[k], b_r.at[k], (flip(s, order[k]), t))

    def experts(g, hooks):
        hooks = list(hooks)
        block = rows[g * group : (g + 1) * group].reshape(group_rows, model)
        f_tile = min(256, f_width)
        for j in range(f_width // f_tile):
            cols = slice(j * f_tile, (j + 1) * f_tile)
            gate = jnp.dot(block, wg[:, cols], preferred_element_type=jnp.float32)
            up = jnp.dot(block, wu[:, cols], preferred_element_type=jnp.float32)
            hid[:, cols] = (gate / (1.0 + jnp.exp(-gate)) * up).astype(jnp.bfloat16)
            if hooks:
                hooks.pop(0)()
        if g == 0:
            weight_copies[3].wait()
        for j in range(model // tile):
            cols = slice(j * tile, (j + 1) * tile)
            down = jnp.dot(hid[...], wd[:, cols], preferred_element_type=jnp.float32)
            down = down.astype(jnp.bfloat16).reshape(group, n_y, 2, capacity, tile)
            for core in range(2):
                for far in range(n_y):
                    eo[core, far, g * group : (g + 1) * group, :, cols] = down[:, far, core]
            if hooks:
                hooks.pop(0)()
        for hook in hooks:
            hook()

    for k in range(group):
        forward(k)
        if k:
            dispatch(window + k - 1)
    dispatch(n_sp - 1)
    for k in range(group):
        relay(k)
    for k in range(group):
        settle(k)
    weight_copies[1].wait()
    weight_copies[2].wait()
    late = range(group, n_sp)
    experts(
        0,
        [functools.partial(forward, k) for k in late] + [functools.partial(relay, k) for k in late],
    )
    give_pair(0)
    for k in late:
        settle(k)
    nothing = lambda: None
    early = list(range(group - 1, -1, -1))
    experts(
        1,
        [functools.partial(start_pairs, 0, early), nothing, nothing, nothing]
        + [functools.partial(return_next, i, early) for i in range(group)],
    )
    give_pair(1)
    start_pairs(1, late)
    for i in range(group):
        return_next(i, late)
    for k in range(1, n_sp):
        arrive(ret.at[k], b_r.at[k])
    high = combiner.astype(jnp.bfloat16)
    rest = combiner - high.astype(jnp.float32)
    middle_part = rest.astype(jnp.bfloat16)
    low = (rest - middle_part.astype(jnp.float32)).astype(jnp.bfloat16)
    returned = ret[...].reshape(total_slots, model)
    routed = jnp.zeros((own, model), jnp.float32)
    for piece in (high, middle_part, low):
        routed = routed + lax.dot_general(
            piece, returned, (((0,), (0,)), ((), ())), preferred_element_type=jnp.float32
        )
    out_ref[...] = mid[...] + routed
    for copy in pending:
        copy.wait_send()


def head_frequency():
    quarter = HEAD_WIDTH // 4
    frequency = ROPE_BASE ** (-np.arange(quarter, dtype=np.float32) / quarter)
    return jnp.asarray(np.tile(frequency, 4).reshape(1, HEAD_WIDTH), jnp.float32)


def local(
    x_resid,
    query_proj,
    projected_key_heads,
    projected_value_heads,
    query_gain,
    key_norm_gain,
    out_weight,
    ffn_gain,
    routing,
    route_scores,
    expert_gate,
    expert_up,
    expert_down,
):
    n_sp, n_tp = lax.axis_size("sp"), lax.axis_size("tp")
    own, model = x_resid.shape
    experts_all = n_sp * expert_gate.shape[0]
    capacity = max(2, 2 * own * TOP // experts_all)
    if capacity % 16 or n_tp & (n_tp - 1) or n_sp & (n_sp - 1) or n_tp < 2 or n_sp < 4 or expert_gate.shape[0] != 1:
        return local_plain(
            x_resid,
            query_proj,
            projected_key_heads,
            projected_value_heads,
            query_gain,
            key_norm_gain,
            out_weight,
            ffn_gain,
            routing,
            route_scores,
            expert_gate,
            expert_up,
            expert_down,
        )
    seq_rows, q_width = query_proj.shape
    kv_width = projected_key_heads.shape[1]
    kv_heads = kv_width // HEAD_WIDTH
    groups = q_width // kv_width
    f_width = expert_gate.shape[2]
    n_y = n_tp // 2
    bf16 = jnp.bfloat16
    dma = pltpu.SemaphoreType.DMA
    vmem = pl.BlockSpec(memory_space=pltpu.VMEM)
    hbm = pl.BlockSpec(memory_space=pl.ANY)
    return pl.pallas_call(
        functools.partial(layer_kernel, n_sp, n_tp, capacity),
        out_shape=jax.ShapeDtypeStruct((own, model), jnp.float32),
        in_specs=[vmem] * 10 + [hbm] * 4,
        out_specs=vmem,
        scratch_shapes=[
            pltpu.VMEM((n_sp, seq_rows, kv_width), bf16),
            pltpu.VMEM((n_sp, seq_rows, kv_width), bf16),
            pltpu.VMEM((kv_heads, groups * seq_rows, HEAD_WIDTH), bf16),
            pltpu.VMEM((seq_rows, q_width), bf16),
            pltpu.VMEM((n_tp, own, model), bf16),
            pltpu.VMEM((n_tp, own, model), bf16),
            pltpu.VMEM((own, model), jnp.float32),
            pltpu.VMEM((n_sp, capacity, model), bf16),
            pltpu.VMEM((n_sp, n_tp, capacity, model), bf16),
            pltpu.VMEM((n_sp // 2 * n_tp * capacity, f_width), bf16),
            pltpu.VMEM((2, n_y, n_sp, capacity, model), bf16),
            pltpu.VMEM((n_y, n_sp, capacity, model), bf16),
            pltpu.VMEM((n_y, n_sp, capacity, model), bf16),
            pltpu.VMEM((n_y, n_sp, capacity, model), bf16),
            pltpu.VMEM((n_sp, capacity, model), bf16),
            pltpu.VMEM((n_sp, capacity, model), bf16),
            pltpu.VMEM(out_weight.shape, bf16),
            pltpu.VMEM(expert_gate.shape[1:], bf16),
            pltpu.VMEM(expert_up.shape[1:], bf16),
            pltpu.VMEM(expert_down.shape[1:], bf16),
            dma((4,)),
            dma((n_sp,)),
            dma((n_sp,)),
            dma((n_sp,)),
            dma((n_sp,)),
            dma((n_tp,)),
            dma((n_tp,)),
            dma((n_sp,)),
            dma((n_sp, n_tp)),
            dma((n_sp, n_y)),
            dma((n_sp, n_y)),
            dma((2,)),
            dma((2,)),
            dma((n_sp, n_y)),
            dma((n_sp, n_y)),
            dma((n_sp,)),
            dma((n_sp,)),
        ],
        compiler_params=pltpu.CompilerParams(
            collective_id=0, has_side_effects=True, vmem_limit_bytes=56 * 1024 * 1024
        ),
    )(
        query_proj,
        projected_key_heads,
        projected_value_heads,
        head_frequency(),
        query_gain.reshape(1, -1),
        key_norm_gain.reshape(1, -1),
        x_resid,
        ffn_gain.reshape(1, -1),
        routing.T,
        route_scores.T,
        out_weight,
        expert_gate,
        expert_up,
        expert_down,
    ).astype(bf16)


def solution(mesh):
    in_specs = (
        P(("sp", "tp"), None),
        P("sp", "tp"),
        P("sp", "tp"),
        P("sp", "tp"),
        P(),
        P(),
        P("tp", None),
        P(),
        P(("sp", "tp"), None),
        P(("sp", "tp"), None),
        P("sp", None, "tp"),
        P("sp", None, "tp"),
        P("sp", "tp", None),
    )
    out_specs = P(("sp", "tp"), None)
    return jax.shard_map(local, mesh=mesh, in_specs=in_specs, out_specs=out_specs, check_vma=False)
```
